256 devices in a mesh: ep: 64 (over z, x, core), tp: 4 (over y).
Axes of the slice: x: 4, y: 4, z: 8, core: 2. Of those that a mesh axis runs over, the one named last changes fastest.
Arguments:
- query_rows: bfloat16 [12288, 1024], P('ep', 'tp'), may hold values from -8 to 8
- key_rows: bfloat16 [12288, 1024], P('ep', 'tp'), may hold values from -8 to 8
- value_rows: bfloat16 [12288, 1024], P('ep', 'tp'), may hold values from -6 to 6
- lambdas: float32 [8], P('tp'), may hold values from 0.3 to 0.8
- head_gain: float32 [128], replicated, may hold values from 0.1 to 1.9
- w_out: bfloat16 [1024, 2048], replicated, may hold values from -0.1875 to 0.1875
- moe_rows: bfloat16 [32768, 2048], P('ep'), may hold values from -6 to 6
- ffn_gain: float32 [2048], replicated, may hold values from 0.1 to 1.9
- routes: int32 [32768, 2], P('ep'), may hold values from 0 to 63, all different within a row; in each aligned block of 128 rows (0 to 127, 128 to 255, ...) at most 8 rows name the same one
- group_logits: float32 [32768, 4], P('ep'), may hold values from -8 to 8
- pick_logits: float32 [32768, 2], P('ep'), may hold values from -8 to 8
- w_gate: bfloat16 [64, 2048, 1024], P('ep', None, 'tp'), may hold values from -0.125 to 0.125
- w_up: bfloat16 [64, 2048, 1024], P('ep', None, 'tp'), may hold values from -0.125 to 0.125
- w_down: bfloat16 [64, 1024, 2048], P('ep', 'tp'), may hold values from -0.75 to 0.75
Outputs:
- mixer_out: bfloat16 [12288, 2048], P(('ep', 'tp'))
- moe_out: bfloat16 [32768, 2048], P(('ep', 'tp'))
The draws below stay inside these ranges and needn't reach their ends.
Inputs may be any that keep to these rules, and one draw needn't show every extreme that they name: `routes`: each row names 2 different experts. In each aligned block of 128 rows (the rows of one device) no expert is named by more than 8 rows; some expert is named by exactly 8 rows of a block.
All inputs are finite; a program needn't handle non-finite values.
Results may differ from the reference program's by a relative error of at most 0.015.
Values may be sent and summed in bfloat16 or wider, within the bound.
No kernel may reach another device: no remote copies, remote signals or barrier semaphores. Data moves between devices by JAX's collectives and lax.ppermute only.
A program may use at most 128 MiB of HBM per device.

```python
import math
import jax
import jax.numpy as jnp
import numpy as np
from jax import lax

D = 2048
HEADS = 8
HEAD_QK = 64
HEAD_V = 128
FFE = 1024
GROUPS = 4
TOP = 2
TOKQ = 128
EXPERTS = 64
CAP = 8
TOKA = 12288
TOKB = 32768
N_EP = 64
N_TP = 4


def drawn_pair(key):
    base = jax.random.fold_in(key, 41)
    first, second = jax.random.split(base, 2)
    columns = HEADS * 2 * HEAD_QK
    queries = jnp.clip(jax.random.normal(first, (TOKA, columns), jnp.float32) * 1.3, -6.0, 6.0)
    keys = jnp.clip(jax.random.normal(second, (TOKA, columns), jnp.float32) * 1.3, -6.0, 6.0)
    return (queries, keys)


def draw_query_rows(key, part):
    return drawn_pair(key)[0].astype(jnp.bfloat16)


def draw_key_rows(key, part):
    return drawn_pair(key)[1].astype(jnp.bfloat16)


def steps_of(rng, extent, shards, least, largest):
    factor_of, own = 1.0, jax.random.fold_in(rng, 6)
    for axis_at, shards_of in shards:
        heights = jnp.exp(jax.random.uniform(jax.random.fold_in(own, axis_at), (shards_of,), jnp.float32, least / len(shards), largest / len(shards)))
        factor_of = factor_of * jnp.repeat(heights, extent[axis_at] // shards_of).reshape([-1 if axis == axis_at else 1 for axis in range(len(extent))])
    return factor_of


def routed_block(own_key, own, number, rows, count, top, reach, lean):
    order = jax.random.permutation(own_key, count)
    crowded, usual = shares(count, rows * top, reach, lean, True), shares(count, rows * top, reach, lean, False)
    places = jnp.arange(count)

    def named(sizes, offset_by):
        used = int((sizes > 0).sum())
        fixed = max(1, used // 4)
        moved = fixed + (places - fixed + offset_by * (used - fixed)) % max(1, count - fixed)
        return jnp.zeros((count,), jnp.int32).at[order[jnp.where(places < fixed, places, moved)]].set(jnp.asarray(sizes, jnp.int32))

    sizes = jnp.where(number % 4 == 0, named(crowded, number // 4), named(usual, number - number // 4 - 1))
    mixed = jax.random.permutation(jax.random.fold_in(own, 3), count)
    donor, taker = mixed[0:count // 2 * 2:2], mixed[1:count // 2 * 2:2]
    margin = jnp.minimum(sizes[donor] - 1, reach - sizes[taker]) // 2
    margin = jnp.where((donor == order[0]) | (taker == order[0]) | (sizes[taker] == 0), 0, jnp.maximum(margin, 0))
    moved = jax.random.randint(jax.random.fold_in(own, 4), (count // 2,), 0, 1 << 20) % (margin + 1)
    sizes = sizes.at[donor].add(-moved).at[taker].add(moved)
    members = jnp.searchsorted(jnp.cumsum(sizes), jnp.arange(rows * top), side="right").astype(jnp.int32)
    table = members.reshape(top, rows).T
    table = table[jax.random.permutation(jax.random.fold_in(own, 1), rows)]
    offset_by = jax.random.randint(jax.random.fold_in(own, 2), (rows, 1), 0, top)
    return jnp.take_along_axis(table, (jnp.arange(top)[None, :] + offset_by) % top, axis=1)


def shares(amount, total, bound, skew, full):
    weights = [(1 << 20) // math.isqrt(rank ** skew) + 1 for rank in range(1, amount + 1)]
    largest = bound if full else min(bound, max(-(-total // amount), total * weights[0] // sum(weights)))
    least = 1 if total - largest >= amount - 1 else 0
    given, rest = [largest] + [least] * (amount - 1), total - largest - least * (amount - 1)
    while rest > 0:
        movable = [i for i in range(1, amount) if given[i] < largest] or [i for i in range(1, amount) if given[i] < bound]
        pool, left = sum([weights[i] for i in movable]), rest
        for i in movable:
            addition = min(bound - given[i], max(1, left * weights[i] // pool), rest)
            given[i] = given[i] + addition
            rest = rest - addition
    return np.array(given)


def scatter_about(own_key, extent, width, most, cuts=(), kind=jnp.bfloat16):
    level = steps_of(own_key, extent, cuts, -0.22, 0.18) if cuts else 1.0
    drawn = jax.random.normal(own_key, extent, jnp.float32) * width * level
    return jnp.minimum(jnp.maximum(drawn, -most), most).astype(kind)


def setup_inputs(seed: int = 0) -> dict:
    key_list = jax.random.split(jax.random.key(seed), 15)
    query_rows = draw_query_rows(jax.random.fold_in(key_list[14], 71), 0)
    key_rows = draw_key_rows(jax.random.fold_in(key_list[14], 71), 0)
    value_rows = scatter_about(key_list[2], (TOKA, HEADS * HEAD_V), 1.0, 6.0, ((0, 64), (1, 4)))
    lambdas = jnp.clip(0.3 + 0.5 * jax.random.uniform(key_list[3], (HEADS,), jnp.float32) ** steps_of(key_list[3], (HEADS,), ((0, 4),), -0.2, 0.2), 0.3, 0.8)
    head_gain = jnp.clip(1.0 + 0.18 * jax.random.normal(key_list[4], (HEAD_V,), jnp.float32), 0.1, 1.9)
    w_out = scatter_about(key_list[5], (HEADS * HEAD_V, D), (HEADS * HEAD_V) ** -0.5, 0.1875)
    moe_rows = scatter_about(key_list[6], (TOKB, D), 1.0, 6.0, ((0, 64),))
    ffn_gain = jnp.clip(1.0 + 0.18 * jax.random.normal(key_list[7], (D,), jnp.float32), 0.1, 1.9)
    routes_keys = jax.random.split(jax.random.fold_in(key_list[8], 1), TOKB // TOKQ)
    routes_turns = jax.random.permutation(jax.random.fold_in(key_list[8], 3), TOKB // TOKQ)
    routes = jax.vmap(lambda own, number: routed_block(jax.random.fold_in(key_list[8], 2), own, number, TOKQ, EXPERTS, TOP, CAP, 1))(routes_keys, routes_turns).reshape((TOKB, TOP))
    group_logits = scatter_about(key_list[9], (TOKB, GROUPS), 2.0, 8.0, ((0, 64),), jnp.float32)
    pick_logits = scatter_about(key_list[10], (TOKB, TOP), 1.5, 8.0, ((0, 64),), jnp.float32)
    w_gate = scatter_about(key_list[11], (EXPERTS, D, FFE), D ** -0.5, 0.125, ((0, 64), (2, 4)))
    w_up = scatter_about(key_list[12], (EXPERTS, D, FFE), D ** -0.5, 0.125, ((0, 64), (2, 4)))
    w_down = scatter_about(key_list[13], (EXPERTS, FFE, D), (FFE // 16) ** -0.5, 0.75, ((0, 64), (1, 4)))
    return dict(query_rows=query_rows, key_rows=key_rows, value_rows=value_rows, lambdas=lambdas, head_gain=head_gain, w_out=w_out, moe_rows=moe_rows, ffn_gain=ffn_gain, routes=routes, group_logits=group_logits, pick_logits=pick_logits, w_gate=w_gate, w_up=w_up, w_down=w_down)


EPS = 1e-06
HEAD_SCALE = 0.8

def rms_rows(values, gain):
    squared = lax.optimization_barrier(jnp.mean(values * values, axis=-1, keepdims=True))
    return values * lax.rsqrt(squared + EPS) * gain

def attend(query_rows, key_rows, value_rows, lambdas, head_gain):
    token_count = query_rows.shape[0]
    block_rows = math.gcd(token_count, 128)
    keys = key_rows.astype(jnp.float32).reshape(token_count, HEADS, 2, HEAD_QK)
    values = value_rows.astype(jnp.float32).reshape(token_count, HEADS, HEAD_V)
    queries = query_rows.astype(jnp.float32).reshape(token_count // block_rows, block_rows, HEADS, 2, HEAD_QK)

    def one_block(query_block):
        scores = jnp.einsum('qhmd,khmd->hmqk', query_block, keys, precision=lax.Precision.HIGHEST) * HEAD_QK ** (-0.5)
        weights = jnp.exp(scores - lax.optimization_barrier(jnp.max(scores, axis=-1, keepdims=True)))
        totals = lax.optimization_barrier(jnp.sum(weights, axis=-1))
        rounded = lax.optimization_barrier(weights.astype(jnp.bfloat16)).astype(jnp.float32)
        sums = jnp.einsum('hmqk,khv->hmqv', rounded, values, precision=lax.Precision.HIGHEST)
        per_head = sums[:, 0] / totals[:, 0, :, None] - lambdas[:, None, None] * sums[:, 1] / totals[:, 1, :, None]
        normed = rms_rows(per_head, head_gain) * HEAD_SCALE
        return jnp.transpose(normed, (1, 0, 2)).reshape(block_rows, HEADS * HEAD_V).astype(jnp.bfloat16)
    return lax.map(one_block, queries).reshape(token_count, HEADS * HEAD_V)

def experts_part(moe_rows, ffn_gain, routes, group_logits, pick_logits, w_gate, w_up, w_down):
    model_width = moe_rows.shape[1]
    quarters = N_EP * N_TP
    normed = rms_rows(moe_rows.astype(jnp.float32), ffn_gain).astype(jnp.bfloat16)
    flattened = routes.reshape(quarters, TOKQ * TOP)
    onehot = (flattened[..., None] == jnp.arange(EXPERTS, dtype=jnp.int32)).astype(jnp.int32)
    before = jnp.cumsum(onehot, axis=1) - onehot
    ranking = lax.optimization_barrier(jnp.sum(before * onehot, axis=-1))
    slots = (flattened * quarters + jnp.arange(quarters, dtype=jnp.int32)[:, None]) * CAP + ranking
    source_rows = jnp.repeat(jnp.arange(TOKB, dtype=jnp.int32), TOP)
    buffer_rows = jnp.zeros((EXPERTS * quarters * CAP, model_width), jnp.bfloat16)
    buffer_rows = buffer_rows.at[slots.reshape(-1)].set(normed[source_rows])
    buffer_rows = buffer_rows.reshape(EXPERTS, quarters * CAP, model_width)
    unit_block = FFE // N_TP

    def run_expert(packed):
        expert_rows, gate_weight, up_weight, down_weight = packed
        gate_part = jnp.dot(expert_rows, gate_weight, preferred_element_type=jnp.float32)
        up_part = jnp.dot(expert_rows, up_weight, preferred_element_type=jnp.float32)
        hidden = (jax.nn.silu(gate_part) * up_part).astype(jnp.bfloat16)
        split_hidden = hidden.astype(jnp.float32).reshape(-1, N_TP, unit_block)
        split_down = down_weight.astype(jnp.float32).reshape(N_TP, unit_block, model_width)
        parts = jnp.einsum('rnf,nfd->nrd', split_hidden, split_down, precision=lax.Precision.HIGHEST)
        parts = lax.optimization_barrier(parts.astype(jnp.bfloat16)).astype(jnp.float32)
        return lax.optimization_barrier(jnp.sum(parts, axis=0)).astype(jnp.bfloat16)
    outputs = lax.map(run_expert, (buffer_rows, w_gate, w_up, w_down))
    picked = outputs.reshape(-1, model_width)[slots.reshape(-1)].reshape(TOKB, TOP, model_width)
    group_prob = jax.nn.softmax(group_logits, axis=-1)
    group_index = routes // (EXPERTS // GROUPS)
    matches = (group_index[..., None] == jnp.arange(GROUPS, dtype=jnp.int32)).astype(jnp.float32)
    group_share = lax.optimization_barrier(jnp.sum(group_prob[:, None, :] * matches, axis=-1))
    gate_values = group_share * jax.nn.softmax(pick_logits, axis=-1)
    return lax.optimization_barrier(jnp.sum(gate_values[..., None] * picked.astype(jnp.float32), axis=1)).astype(jnp.bfloat16)

def reference(query_rows, key_rows, value_rows, lambdas, head_gain, w_out, moe_rows, ffn_gain, routes, group_logits, pick_logits, w_gate, w_up, w_down):
    attended = attend(query_rows, key_rows, value_rows, lambdas, head_gain)
    mixer_out = jnp.dot(attended, w_out, preferred_element_type=jnp.float32).astype(jnp.bfloat16)
    moe_out = experts_part(moe_rows, ffn_gain, routes, group_logits, pick_logits, w_gate, w_up, w_down)
    return (mixer_out, moe_out)
```

```python
import jax
import jax.numpy as jnp
from jax import lax
from jax.experimental import pallas as pl
from jax.experimental.pallas import tpu as pltpu
from jax.sharding import Mesh
from jax.sharding import PartitionSpec as P

EPS = 1e-06
HEAD_SCALE = 0.8
LOG2E = 1.4426950408889634
BF16 = jnp.bfloat16
F32 = jnp.float32
EP = ("z", "x", "c")


def shifted(size, by):
    return [(i, (i + by) % size) for i in range(size)]


def sent(x, axis, by):
    return lax.ppermute(x, axis, shifted(lax.axis_size(axis), by))


def ring_gather(block, axis):
    size = lax.axis_size(axis)
    blocks, right, left = [block], block, block
    for step in range(1, size // 2 + 1):
        if 2 * step < size:
            right = sent(right, axis, 1)
            left = sent(left, axis, -1)
            blocks += [right, left]
        else:
            half = block.shape[0] // 2
            far_right = sent(right[:half], axis, 1)
            far_left = sent(left[half:], axis, -1)
            blocks.append(jnp.concatenate([far_right, far_left], axis=0))
    return blocks


def dispatch_body(cap, groups, where_ref, rows_ref, gain_ref, routes_ref, group_ref, pick_ref, out_ref, hi_ref, lo_ref):
    rows = rows_ref[...].astype(F32)
    squared = jnp.mean(rows * rows, axis=-1, keepdims=True)
    normed = (rows * lax.rsqrt(squared + EPS) * gain_ref[...]).astype(BF16)
    count = rows.shape[0]
    slots = out_ref.shape[0]
    experts = slots // cap
    per_group = experts // groups
    expert_ids = lax.broadcasted_iota(jnp.int32, (count, experts), 1)

    def upright(ref):
        values = ref[...].astype(F32)
        fill = jnp.zeros((8 - values.shape[0], count), F32)
        return jnp.concatenate([values, fill], axis=0).T

    named = upright(routes_ref).astype(jnp.int32)
    first, second = named[:, 0:1], named[:, 1:2]
    hot_first = (expert_ids == first).astype(F32)
    hot_second = (expert_ids == second).astype(F32)
    earlier = (
        lax.broadcasted_iota(jnp.int32, (count, count), 1)
        < lax.broadcasted_iota(jnp.int32, (count, count), 0)
    ).astype(F32).astype(BF16)
    before_first = jnp.dot(earlier, hot_first.astype(BF16), preferred_element_type=F32)
    before_second = jnp.dot(earlier, hot_second.astype(BF16), preferred_element_type=F32)
    before_second = before_second + jnp.sum(hot_first, axis=0, keepdims=True)
    rank_first = jnp.sum(before_first * hot_first, axis=1, keepdims=True).astype(jnp.int32)
    rank_second = jnp.sum(before_second * hot_second, axis=1, keepdims=True).astype(jnp.int32)
    slot_ids = lax.broadcasted_iota(jnp.int32, (count, slots), 1)
    at_first = slot_ids == first * cap + rank_first
    at_second = slot_ids == second * cap + rank_second
    placed = jnp.where(at_first | at_second, 1.0, 0.0).astype(BF16)
    out_ref[...] = lax.dot_general(
        placed, normed, (((0,), (0,)), ((), ())), preferred_element_type=F32
    ).astype(BF16)

    logits = upright(group_ref)[:, :groups]
    group_exp = jnp.exp(logits - jnp.max(logits, axis=-1, keepdims=True))
    group_prob = group_exp / jnp.sum(group_exp, axis=-1, keepdims=True)
    picks = upright(pick_ref)[:, :2]
    pick_exp = jnp.exp(picks - jnp.max(picks, axis=-1, keepdims=True))
    pick_prob = pick_exp / jnp.sum(pick_exp, axis=-1, keepdims=True)
    group_ids = lax.broadcasted_iota(jnp.int32, (count, groups), 1)

    def share(expert):
        inside = (expert >= group_ids * per_group) & (expert < (group_ids + 1) * per_group)
        return jnp.sum(jnp.where(inside, group_prob, 0.0), axis=-1, keepdims=True)

    gates = jnp.where(at_first, share(first) * pick_prob[:, 0:1], 0.0)
    gates = gates + jnp.where(at_second, share(second) * pick_prob[:, 1:2], 0.0)
    high = gates.astype(BF16)
    hi_ref[...] = high
    lo_ref[...] = (gates - high.astype(F32)).astype(BF16)


def dispatch(moe_rows, ffn_gain, routes, group_logits, pick_logits, quarters, quarter, experts):
    rows, width = moe_rows.shape[0] // quarters, moe_rows.shape[1]
    top, groups = routes.shape[1], group_logits.shape[1]
    cap = max(2, 2 * top * rows // experts)

    def cut(lines):
        return pl.BlockSpec((lines, rows), lambda i, where: (0, where[0]))

    def whole(*shape):
        return pl.BlockSpec(shape, lambda i, where: (0,) * len(shape))

    return pl.pallas_call(
        lambda *refs: dispatch_body(cap, groups, *refs),
        grid_spec=pltpu.PrefetchScalarGridSpec(
            num_scalar_prefetch=1,
            grid=(1,),
            in_specs=[
                pl.BlockSpec((rows, width), lambda i, where: (where[0], 0)),
                whole(1, width),
                cut(top),
                cut(groups),
                cut(top),
            ],
            out_specs=[whole(experts * cap, width), whole(rows, experts * cap), whole(rows, experts * cap)],
        ),
        out_shape=[
            jax.ShapeDtypeStruct((experts * cap, width), BF16),
            jax.ShapeDtypeStruct((rows, experts * cap), BF16),
            jax.ShapeDtypeStruct((rows, experts * cap), BF16),
        ],
        name="dispatch",
    )(quarter.astype(jnp.int32).reshape(1), moe_rows, ffn_gain.reshape(1, -1), routes.T, group_logits.T, pick_logits.T)


def attend_body(n_q, n_kv, scale, *refs):
    q_refs, kv_refs = refs[:n_q], refs[n_q : n_q + n_kv]
    out_refs = refs[n_q + n_kv : n_q + n_kv + n_q]
    qt, keys, vt, scores, peak = refs[n_q + n_kv + n_q :]
    q_rows, pair = q_refs[0].shape
    kv_rows = kv_refs[0].shape[0]
    half = pair // 2
    n_chunks, head_v, chunk = vt.shape
    per_chunk = chunk // kv_rows
    wide = 2 * q_rows
    zero = jnp.zeros((half, q_rows), BF16)
    for i in range(n_q):
        scaled = (q_refs[i][...].astype(F32) * scale).T
        high = scaled.astype(BF16)
        low = (scaled - high.astype(F32)).astype(BF16)
        first = jnp.concatenate([high[:half], zero, low[:half], zero], axis=0)
        second = jnp.concatenate([zero, high[half:], zero, low[half:]], axis=0)
        qt[i] = jnp.concatenate([first, second], axis=1)
    for i in range(n_kv):
        at, sub = divmod(i, per_chunk)
        keys[at, sub * kv_rows : (sub + 1) * kv_rows, :] = kv_refs[i][:, :pair]
        vt[at, :, sub * kv_rows : (sub + 1) * kv_rows] = kv_refs[i][:, pair:].astype(F32).T.astype(BF16)

    def score(i, slot, c):
        block = keys[c]
        s = jnp.dot(jnp.concatenate([block, block], axis=1), qt[i], preferred_element_type=F32)
        scores[slot, c] = s
        peak[slot] = jnp.maximum(peak[slot], jnp.max(s.reshape(chunk // 8, 8, wide), axis=0))

    def absorb(slot, c, top, acc, total):
        p = jnp.exp2(scores[slot, c] - top)
        total = total + jnp.sum(p.reshape(chunk // 8, 8, wide), axis=0)
        acc[0:head_v, :] = acc[0:head_v, :] + jnp.dot(vt[c], p.astype(BF16), preferred_element_type=F32)
        return total

    for i in range(n_q + 1):
        slot, other = i % 2, (i + 1) % 2
        if i < n_q:
            peak[slot] = jnp.full((8, wide), -jnp.inf, F32)
        if i > 0:
            acc = out_refs[i - 1]
            top = jnp.max(peak[other], axis=0, keepdims=True)
            acc[0:head_v, :] = jnp.zeros((head_v, wide), F32)

        def step(c, total, i=i, slot=slot, other=other):
            if i < n_q:
                score(i, slot, c)
            if i > 0:
                total = absorb(other, c, top, acc, total)
            return total

        total = lax.fori_loop(0, n_chunks, step, jnp.zeros((8, wide), F32))
        if i > 0:
            acc[head_v : head_v + 1, :] = top
            acc[head_v + 1 : head_v + 2, :] = jnp.sum(total, axis=0, keepdims=True)
            acc[head_v + 2 :, :] = jnp.zeros((acc.shape[0] - head_v - 2, wide), F32)


def attend(queries, key_values, scale):
    n_q, n_kv = len(queries), len(key_values)
    q_rows, pair = queries[0].shape
    kv_rows = key_values[0].shape[0]
    head_v = key_values[0].shape[1] - pair
    per_chunk = 2 if n_kv % 2 == 0 else 1
    n_chunks, chunk, wide = n_kv // per_chunk, kv_rows * per_chunk, 2 * q_rows
    flops = 2 * n_q * wide * n_chunks * chunk * (2 * pair + head_v)
    return pl.pallas_call(
        lambda *refs: attend_body(n_q, n_kv, scale, *refs),
        out_shape=[jax.ShapeDtypeStruct((head_v + 8, wide), F32)] * n_q,
        in_specs=[pl.BlockSpec(memory_space=pltpu.VMEM)] * (n_q + n_kv),
        out_specs=[pl.BlockSpec(memory_space=pltpu.VMEM)] * n_q,
        scratch_shapes=[
            pltpu.VMEM((n_q, 2 * pair, wide), BF16),
            pltpu.VMEM((n_chunks, chunk, pair), BF16),
            pltpu.VMEM((n_chunks, head_v, chunk), BF16),
            pltpu.VMEM((2, n_chunks, chunk, wide), F32),
            pltpu.VMEM((2, 8, wide), F32),
        ],
        cost_estimate=pl.CostEstimate(flops=flops, transcendentals=0, bytes_accessed=8 << 20),
        name="attend",
    )(*queries, *key_values)


def merge(parts, head_v, count, lambdas, head_gain, core):
    tops = [p[head_v : head_v + 1] for p in parts]
    top = jnp.maximum(jnp.maximum(tops[0], tops[1]), jnp.maximum(tops[2], tops[3]))
    weights = [jnp.exp2(t - top) for t in tops]
    total = sum(w * p[head_v + 1 : head_v + 2] for w, p in zip(weights, parts))
    averaged = sum(w * p[:head_v] for w, p in zip(weights, parts)) / total
    own_lambda = lax.dynamic_slice_in_dim(lambdas, core, 1, 0)
    per_head = averaged[:, :count] - own_lambda * averaged[:, count:]
    squared = jnp.mean(per_head * per_head, axis=0, keepdims=True)
    attended = per_head * lax.rsqrt(squared + EPS) * head_gain[:, None] * HEAD_SCALE
    return attended.astype(BF16).T


def mixer(query_rows, key_rows, value_rows, lambdas, head_gain, w_out):
    core = lax.axis_index("c")
    rows = query_rows.shape[0]
    heads = lax.axis_size("c")
    pair = query_rows.shape[1] // heads
    head_v = value_rows.shape[1] // heads

    def head_of(which):
        cut = [
            lax.dynamic_slice_in_dim(query_rows, which * pair, pair, 1),
            lax.dynamic_slice_in_dim(key_rows, which * pair, pair, 1),
            lax.dynamic_slice_in_dim(value_rows, which * head_v, head_v, 1),
        ]
        return jnp.concatenate(cut, axis=1)

    kept = head_of(core)
    met = sent(head_of(1 - core), "c", 1)
    is_first = core == 0
    both = jnp.concatenate([jnp.where(is_first, kept, met), jnp.where(is_first, met, kept)], axis=0)
    own_queries = both[:, :pair]
    own_kv = both[:, pair:]

    kv_blocks = ring_gather(own_kv, "z")
    hops = [1, -1, 2]
    q_blocks = [own_queries] + [sent(own_queries, "x", h) for h in hops]
    parts = attend(q_blocks, kv_blocks, (pair // 2) ** (-0.5) * LOG2E)
    parts = [parts[0]] + [sent(p, "x", -h) for h, p in zip(hops, parts[1:])]

    attended = merge(parts, head_v, own_queries.shape[0], lambdas, head_gain, core)

    quarters = lax.axis_size("tp")
    share = rows // quarters
    kept = lax.dynamic_slice_in_dim(attended, core * rows, rows, 0)
    met = sent(lax.dynamic_slice_in_dim(attended, (1 - core) * rows, rows, 0), "c", 1)
    pair_rows = jnp.concatenate([jnp.where(is_first, kept, met), jnp.where(is_first, met, kept)], axis=1)
    gathered = lax.all_gather(pair_rows, "tp", axis=0, tiled=False)
    mine = lax.dynamic_slice_in_dim(gathered, lax.axis_index("tp") * share, share, 1)
    mine = jnp.transpose(mine, (1, 0, 2)).reshape(share, quarters * heads * head_v)
    return jnp.dot(mine, w_out, preferred_element_type=F32).astype(BF16)


def weight_ring(w_gate, w_up, w_down):
    middle = w_down.shape[0] // 2
    near = []
    for w in (w_gate, w_up, w_down[:middle], w_down[middle:]):
        near.append((w, sent(w, "tp", 1), sent(w, "tp", -1)))
    gate = (*near[0], sent(near[0][1], "tp", 1))
    up = (*near[1], sent(near[1][2], "tp", -1))
    top = (*near[2], sent(near[2][1], "tp", 1))
    bottom = (*near[3], sent(near[3][2], "tp", -1))
    return gate, up, (w_down, *[half for pair in zip(top[1:], bottom[1:]) for half in pair])


def hidden_body(rows_ref, *refs):
    gate_refs, up_refs = refs[:4], refs[4:8]
    out_ref, rows, both, sems = refs[8:]
    units = gate_refs[0].shape[1]
    moves = [pltpu.make_async_copy(rows_ref, rows, sems.at[0])]
    for i in range(4):
        for side, ref in enumerate((gate_refs[i], up_refs[i])):
            target = both.at[i, :, pl.ds(side * units, units)]
            moves.append(pltpu.make_async_copy(ref, target, sems.at[1 + 2 * i + side]))
    for move in moves:
        move.start()
    moves[0].wait()
    for i in range(4):
        moves[1 + 2 * i].wait()
        moves[2 + 2 * i].wait()
        parts = jnp.dot(rows[...], both[i], preferred_element_type=F32)
        gate, up = parts[:, :units], parts[:, units:]
        out_ref[:, i * units : (i + 1) * units] = (gate / (1.0 + jnp.exp(-gate)) * up).astype(BF16)


def run_hidden(rows, gates, ups):
    count, width = rows.shape
    units = gates[0].shape[1]
    anywhere = pl.BlockSpec(memory_space=pl.ANY)
    return pl.pallas_call(
        hidden_body,
        out_shape=jax.ShapeDtypeStruct((count, 4 * units), BF16),
        in_specs=[anywhere] * 9,
        out_specs=pl.BlockSpec(memory_space=pltpu.VMEM),
        scratch_shapes=[
            pltpu.VMEM((count, width), BF16),
            pltpu.VMEM((4, width, 2 * units), BF16),
            pltpu.SemaphoreType.DMA((9,)),
        ],
        cost_estimate=pl.CostEstimate(flops=16 * count * width * units, transcendentals=0, bytes_accessed=12 << 20),
        name="hidden",
    )(rows, *gates, *ups)


def down_body(n_down, pieces, hidden_ref, *refs):
    down_refs = refs[:n_down]
    out_ref, downs, sems = refs[n_down:]
    piece = out_ref.shape[1] // pieces
    moves = []
    for c in range(pieces):
        at = 0
        for i in range(n_down):
            lines = down_refs[i].shape[0]
            source = down_refs[i].at[:, pl.ds(c * piece, piece)]
            moves.append(pltpu.make_async_copy(source, downs.at[c, pl.ds(at, lines)], sems.at[c, i]))
            at += lines
    for move in moves[: 2 * n_down]:
        move.start()
    for c in range(pieces):
        for move in moves[c * n_down : (c + 1) * n_down]:
            move.wait()
        for move in moves[(c + 2) * n_down : (c + 3) * n_down]:
            move.start()
        out_ref[:, c * piece : (c + 1) * piece] = jnp.dot(
            hidden_ref[...], downs[c], preferred_element_type=F32
        ).astype(BF16)


def run_down(hidden, downs):
    count, units = hidden.shape
    width = downs[0].shape[1]
    n_down, pieces = len(downs), 4
    return pl.pallas_call(
        lambda *refs: down_body(n_down, pieces, *refs),
        out_shape=jax.ShapeDtypeStruct((count, width), BF16),
        in_specs=[pl.BlockSpec(memory_space=pltpu.VMEM)] + [pl.BlockSpec(memory_space=pl.ANY)] * n_down,
        out_specs=pl.BlockSpec(memory_space=pltpu.VMEM),
        scratch_shapes=[
            pltpu.VMEM((pieces, units, width // pieces), BF16),
            pltpu.SemaphoreType.DMA((pieces, n_down)),
        ],
        cost_estimate=pl.CostEstimate(flops=2 * count * width * units, transcendentals=0, bytes_accessed=7 << 20),
        name="down",
    )(hidden, *downs)


def experts(moe_rows, ffn_gain, routes, group_logits, pick_logits, w_gate, w_up, w_down):
    quarters = lax.axis_size("tp")
    expert_count = lax.axis_size(EP)
    gates, ups, downs = weight_ring(w_gate[0], w_up[0], w_down[0])
    outgoing, gate_hi, gate_lo = dispatch(
        moe_rows, ffn_gain, routes, group_logits, pick_logits, quarters, lax.axis_index("tp"), expert_count
    )

    def exchange(x):
        cap = x.shape[0] // expert_count
        moved = lax.all_to_all(x.reshape(expert_count, cap, x.shape[1]), EP, 0, 0, tiled=True)
        return moved.reshape(x.shape)

    arrived = exchange(outgoing)
    hidden = run_hidden(arrived, gates, ups)
    out = run_down(hidden, downs)
    back = exchange(out)
    picked = jnp.dot(gate_hi, back, preferred_element_type=F32)
    picked = picked + jnp.dot(gate_lo, back, preferred_element_type=F32)
    return picked.astype(BF16)


def local(
    query_rows,
    key_rows,
    value_rows,
    lambdas,
    head_gain,
    w_out,
    moe_rows,
    ffn_gain,
    routes,
    group_logits,
    pick_logits,
    w_gate,
    w_up,
    w_down,
):
    moe_out = experts(moe_rows, ffn_gain, routes, group_logits, pick_logits, w_gate, w_up, w_down)
    mixer_out = mixer(query_rows, key_rows, value_rows, lambdas, head_gain, w_out)
    return (mixer_out, moe_out)


def solution(mesh):
    n_ep, n_tp = mesh.shape["ep"], mesh.shape["tp"]
    cores, n_x = 2, 4
    split = Mesh(mesh.devices.reshape(n_ep // (n_x * cores), n_x, cores, n_tp), ("z", "x", "c", "tp"))
    return jax.shard_map(
        local,
        mesh=split,
        in_specs=(
            P(EP, "tp"),
            P(EP, "tp"),
            P(EP, "tp"),
            P("tp"),
            P(),
            P(),
            P(EP, None),
            P(),
            P(EP, None),
            P(EP, None),
            P(EP, None),
            P(EP, None, "tp"),
            P(EP, None, "tp"),
            P(EP, "tp", None),
        ),
        out_specs=(P((*EP, "tp"), None), P((*EP, "tp"), None)),
        check_vma=False,
    )
```
